32 devices in a mesh: fs: 4 (over z), tp: 8 (over y, x, core).
Axes of the slice: x: 2, y: 2, z: 4, core: 2. Of those that a mesh axis runs over, the one named last changes fastest.
Arguments:
- tokens: bfloat16 [1024, 1344], P('fs'), may hold values from -6 to 6
- cotangent: bfloat16 [1024, 1344], P('fs'), may hold values from -8 to 8
- gate_weight: bfloat16 [1344, 3072], P('fs', 'tp'), may hold values from -0.15625 to 0.15625
- up_weight: bfloat16 [1344, 3072], P('fs', 'tp'), may hold values from -0.15625 to 0.15625
- down_weight: bfloat16 [3072, 1344], P('tp', 'fs'), may hold values from -0.109375 to 0.109375
Outputs:
- input_grad: bfloat16 [1024, 1344], P('fs')
- down_grad: float32 [3072, 1344], P('tp', 'fs')
The draws below stay inside these ranges and needn't reach their ends.
All inputs are finite; a program needn't handle non-finite values.
Results may differ from the reference program's by a relative error of at most 0.013.
Values may be sent and summed in bfloat16 or wider, within the bound.
A program may use at most 64 MiB of HBM per device.

```python
import jax
import jax.numpy as jnp
from jax import lax

D = 1344
FF = 3072
TOKENS = 1024
N_TP = 8


def with_spikes(values, key, source, target, blocks, factor):
    owner, partner = [(jnp.arange(values.shape[position]) // (values.shape[position] // blocks)).reshape([-1 if axis == position else 1 for axis in range(values.ndim)]) for position in (source, target)]
    chosen = jax.random.permutation(key, blocks)[partner]
    strong = (owner == chosen) | (owner == (partner + blocks // 2) % blocks)
    return jnp.where(strong, factor * values, values)


def steps_of(stream_key, dims, split, least, largest):
    factor_of, own = 1.0, jax.random.fold_in(stream_key, 6)
    for axis_at, blocks in split:
        heights = jnp.exp(jax.random.uniform(jax.random.fold_in(own, axis_at), (blocks,), jnp.float32, least / len(split), largest / len(split)))
        factor_of = factor_of * jnp.repeat(heights, dims[axis_at] // blocks).reshape([-1 if axis == axis_at else 1 for axis in range(len(dims))])
    return factor_of


def scatter_about(rng, shape, width, limit, split=(), held_as=jnp.bfloat16):
    level = steps_of(rng, shape, split, -0.22, 0.18) if split else 1.0
    values = jax.random.normal(rng, shape, jnp.float32) * width * level
    return jnp.minimum(jnp.maximum(values, -limit), limit).astype(held_as)


def bell_draw_with(key, extent, spread, limit, shards, heavy, dtype=jnp.bfloat16):
    result = spread * jax.random.normal(key, extent, jnp.float32)
    if shards:
        result = result * steps_of(key, extent, shards, -0.22, 0.18)
    return jnp.clip(with_spikes(result, jax.random.fold_in(key, 3), *heavy), -limit, limit).astype(dtype)


def setup_inputs(seed: int = 0) -> dict:
    streams_of = jax.random.split(jax.random.key(seed), 6)
    tokens = scatter_about(streams_of[0], (TOKENS, D), 1.0, 6.0, ((0, 4),))
    cotangent = bell_draw_with(streams_of[1], (TOKENS, D), 1.0, 8.0, ((0, 4),), (0, 1, 4, 2.0))
    gate_weight = scatter_about(streams_of[2], (D, FF), D ** -0.5, 0.15625, ((0, 4), (1, 8)))
    up_weight = scatter_about(streams_of[3], (D, FF), D ** -0.5, 0.15625, ((0, 4), (1, 8)))
    down_weight = scatter_about(streams_of[4], (FF, D), FF ** -0.5, 0.109375, ((0, 8), (1, 4)))
    return dict(tokens=tokens, cotangent=cotangent, gate_weight=gate_weight, up_weight=up_weight, down_weight=down_weight)


def contract_rows(left, right):
    return lax.dot_general(left, right, (((0,), (0,)), ((), ())), preferred_element_type=jnp.float32)


def contract_cols(left, right):
    return lax.dot_general(left, right, (((1,), (1,)), ((), ())), preferred_element_type=jnp.float32)


def reference(tokens, cotangent, gate_weight, up_weight, down_weight):
    gate_pre = jnp.dot(tokens, gate_weight, preferred_element_type=jnp.float32)
    up_pre = jnp.dot(tokens, up_weight, preferred_element_type=jnp.float32)
    sigmoid_gate = jax.nn.sigmoid(gate_pre)
    activated = gate_pre * sigmoid_gate
    hidden = (activated * up_pre).astype(jnp.bfloat16)
    hidden_grad = contract_cols(cotangent, down_weight)
    gate_pre_grad = (hidden_grad * up_pre * sigmoid_gate * (1.0 + gate_pre * (1.0 - sigmoid_gate))).astype(jnp.bfloat16)
    up_pre_grad = (hidden_grad * activated).astype(jnp.bfloat16)
    block_width = FF // N_TP
    summed = jnp.zeros(tokens.shape, jnp.float32)
    for member in range(N_TP):
        lower = member * block_width
        upper = lower + block_width
        partial_value = contract_cols(gate_pre_grad[:, lower:upper], gate_weight[:, lower:upper])
        partial_value = partial_value + contract_cols(up_pre_grad[:, lower:upper], up_weight[:, lower:upper])
        summed = summed + partial_value.astype(jnp.bfloat16).astype(jnp.float32)
    input_grad = summed.astype(jnp.bfloat16)
    down_grad = contract_rows(hidden, cotangent)
    return input_grad, down_grad
```

```python
import functools

import jax
import jax.numpy as jnp
from jax import lax
from jax.experimental import pallas as pl
from jax.experimental.pallas import tpu as pltpu
from jax.sharding import PartitionSpec as P

LANES = 128
SUB = 16
BF16 = jnp.bfloat16
F32 = jnp.float32


def contract_rows(left, right):
    return lax.dot_general(
        left, right, (((0,), (0,)), ((), ())), preferred_element_type=jnp.float32
    )


def contract_cols(left, right):
    return lax.dot_general(
        left, right, (((1,), (1,)), ((), ())), preferred_element_type=jnp.float32
    )


def send_down(hidden, cotangent):
    return lax.psum_scatter(
        contract_rows(cotangent, hidden), "fs", scatter_dimension=0, tiled=True
    ).T


def per_device_plain(tokens, cotangent, gate_weight, up_weight, down_weight):
    whole_gate, whole_up, whole_down = (
        lax.all_gather(gate_weight, "fs", axis=0, tiled=True),
        lax.all_gather(up_weight, "fs", axis=0, tiled=True),
        lax.all_gather(down_weight, "fs", axis=1, tiled=True),
    )
    gate_pre = jnp.dot(tokens, whole_gate, preferred_element_type=jnp.float32)
    up_pre = jnp.dot(tokens, whole_up, preferred_element_type=jnp.float32)
    hidden_grad = contract_cols(cotangent, whole_down)
    sigmoid_gate = jax.nn.sigmoid(gate_pre)
    activated = gate_pre * sigmoid_gate
    hidden = (activated * up_pre).astype(jnp.bfloat16)
    gate_pre_grad = (
        hidden_grad * up_pre * sigmoid_gate * (1.0 + gate_pre * (1.0 - sigmoid_gate))
    ).astype(jnp.bfloat16)
    up_pre_grad = (hidden_grad * activated).astype(jnp.bfloat16)
    partial_value = contract_cols(gate_pre_grad, whole_gate) + contract_cols(up_pre_grad, whole_up)
    input_grad = lax.psum(partial_value.astype(jnp.bfloat16), "tp")
    down_grad = send_down(hidden, cotangent)
    return (input_grad, down_grad)


def kernel(n, tok_ref, cot_ref, gate_ref, up_ref, down_ref, dx_out, dg_out,
           wgu, wd, cot4, dxacc, part, rsr, rss, rx1, rx2, rx3, tx1, tx2, tx3, ybuf,
           ag_send, ag_recv, rs_send, rs_recv, ar_send, ar_recv, loc_sem):
    z = lax.axis_index("fs")
    b = lax.axis_index("tp")
    rows, depth = tok_ref.shape
    shard, ff = gate_ref.shape
    chunks = ff // LANES
    core = lax.rem(b, 2)
    m2 = 2 + 2 * core
    m3 = 6 - m2
    bit2 = lax.rem(b // m2, 2)
    bit3 = lax.rem(b // m3, 2)
    p1 = b + 1 - 2 * core
    p2 = b + m2 * (1 - 2 * bit2)
    p3 = b + m3 * (1 - 2 * bit3)
    has_left = z > 0
    has_right = z < n - 1

    def z_id(step):
        return {"fs": z + step}

    barrier = pltpu.get_barrier_semaphore()
    for partner in (p1, p2, p3):
        pl.semaphore_signal(barrier, inc=1, device_id={"tp": partner},
                            device_id_type=pl.DeviceIdType.MESH)
    for step, there in ((-1, has_left), (1, has_right)):
        @pl.when(there)
        def _():
            pl.semaphore_signal(barrier, inc=1, device_id=z_id(step),
                                device_id_type=pl.DeviceIdType.MESH)
    peers = 3 + lax.div(z + n - 1, n) + lax.div(2 * n - 2 - z, n)
    pl.semaphore_wait(barrier, peers)

    def slot(c, s, kind):
        r = pl.ds(pl.multiple_of(s * shard, SUB), shard)
        if kind == 0:
            return wgu.at[r, pl.ds(2 * c * LANES, LANES)]
        if kind == 1:
            return wgu.at[r, pl.ds((2 * c + 1) * LANES, LANES)]
        return wd.at[s, pl.ds(c * LANES, LANES), :]

    def own(c, kind):
        if kind == 0:
            return gate_ref.at[:, pl.ds(c * LANES, LANES)]
        if kind == 1:
            return up_ref.at[:, pl.ds(c * LANES, LANES)]
        return down_ref.at[pl.ds(c * LANES, LANES), :]

    def ag_copy(src, c, s, kind, side):
        step = 1 if side else -1
        return pltpu.make_async_remote_copy(
            src_ref=src, dst_ref=slot(c, s, kind),
            send_sem=ag_send.at[side, c, s, kind], recv_sem=ag_recv.at[c, s, kind],
            device_id=z_id(step), device_id_type=pl.DeviceIdType.MESH)

    def send_own(c):
        for side, there in ((0, has_left), (1, has_right)):
            @pl.when(there)
            def _():
                for kind in range(3):
                    ag_copy(own(c, kind), c, z, kind, side).start()

    def gather(c):
        for d in range(1, n):
            for side in (0, 1):
                s = z - d if side == 0 else z + d
                here = (z >= d) if side == 0 else (z + d <= n - 1)
                onward = has_right if side == 0 else has_left
                @pl.when(here)
                def _():
                    for kind in range(3):
                        src = slot(c, s, kind)
                        ag_copy(src, c, s, kind, 1 - side).wait_recv()
                        @pl.when(onward)
                        def _():
                            ag_copy(src, c, s, kind, 1 - side).start()

    def local_copy(c, kind):
        return pltpu.make_async_copy(own(c, kind), slot(c, z, kind), loc_sem.at[c, kind])

    send_own(0)
    for c in range(chunks):
        for kind in range(3):
            local_copy(c, kind).start()
    for k in range(n):
        cot4[k] = cot_ref[:, k * shard:(k + 1) * shard]

    def rs_copy(c, k, side):
        return pltpu.make_async_remote_copy(
            src_ref=rss.at[side, c, k], dst_ref=rsr.at[side, c, k],
            send_sem=rs_send.at[side, c, k], recv_sem=rs_recv.at[side, c, k],
            device_id=z_id(1 if side else -1), device_id_type=pl.DeviceIdType.MESH)

    def rs_targets(side):
        return range(n - 1, 0, -1) if side else range(n - 1)

    def rs_start(c):
        for side, end in ((1, z == 0), (0, z == n - 1)):
            @pl.when(end)
            def _():
                for k in rs_targets(side):
                    rss[side, c, k] = part[c, k].astype(BF16)
                    rs_copy(c, k, side).start()

    def rs_mid(c):
        for side, middle in ((1, has_left), (0, has_right)):
            for k in rs_targets(side):
                ahead = (k > z) if side else (k < z)
                @pl.when(jnp.logical_and(middle, ahead))
                def _():
                    rs_copy(c, k, side).wait_recv()
                    rss[side, c, k] = (part[c, k] + rsr[side, c, k].astype(F32)).astype(BF16)
                    rs_copy(c, k, side).start()

    def rs_final(c):
        r = pl.ds(c * LANES, LANES)
        dg_out[r, :] = part[c, z]
        for side, there in ((1, has_left), (0, has_right)):
            @pl.when(there)
            def _():
                rs_copy(c, z, side).wait_recv()
                dg_out[r, :] += rsr[side, c, z].astype(F32)

    def ar_copy(i, src, dst, partner):
        return pltpu.make_async_remote_copy(
            src_ref=src, dst_ref=dst, send_sem=ar_send.at[i], recv_sem=ar_recv.at[i],
            device_id={"tp": partner}, device_id_type=pl.DeviceIdType.MESH)

    half, quarter, eighth = rows // 2, rows // 4, rows // 8
    lo1 = core * half
    other1 = (1 - core) * half
    lo2 = lo1 + bit2 * quarter
    other2 = lo1 + (1 - bit2) * quarter
    lo3 = lo2 + bit3 * eighth
    other3 = lo2 + (1 - bit3) * eighth

    def at(lo, size):
        return pl.ds(pl.multiple_of(lo, SUB), size)

    ar1 = ar_copy(0, tx1, rx1, p1)
    ar2 = ar_copy(1, tx2, rx2, p2)
    ar3 = ar_copy(2, tx3, rx3, p3)

    for c in range(chunks):
        gather(c)
        if c + 1 < chunks:
            send_own(c + 1)
        for kind in range(3):
            local_copy(c, kind).wait()
        w = wgu[:, 2 * c * LANES:(2 * c + 2) * LANES]
        pre = jnp.dot(tok_ref[...], w, preferred_element_type=F32)
        hg = contract_cols(cot4[0], wd[0, c * LANES:(c + 1) * LANES, :])
        for k in range(1, n):
            hg += contract_cols(cot4[k], wd[k, c * LANES:(c + 1) * LANES, :])
        gate_pre, up_pre = pre[:, :LANES], pre[:, LANES:]
        sig = jax.nn.sigmoid(gate_pre)
        act = gate_pre * sig
        hidden = act * up_pre
        dgu = jnp.concatenate(
            [(hg * up_pre * sig * (1.0 + gate_pre * (1.0 - sig))).astype(BF16),
             (hg * act).astype(BF16)], axis=1)
        if c == 0:
            dxacc[...] = contract_cols(dgu, w)
        else:
            dxacc[...] += contract_cols(dgu, w)
        if c == chunks - 1:
            tx1[...] = dxacc[at(other1, half), :].astype(BF16)
            ar1.start()
        hidden_t = hidden.T.astype(BF16)
        for k in range(n):
            part[c, k] = jnp.dot(hidden_t, cot4[k], preferred_element_type=F32)
        rs_start(c)
        if c > 0 and c < chunks - 1:
            rs_mid(c - 1)

    ar1.wait_recv()
    tx2[...] = (dxacc[at(other2, quarter), :]
                + rx1[at(other2 - lo1, quarter), :].astype(F32)).astype(BF16)
    ar2.start()
    dxacc[at(lo2, quarter), :] += rx1[at(lo2 - lo1, quarter), :].astype(F32)
    ar2.wait_recv()
    tx3[...] = (dxacc[at(other3, eighth), :]
                + rx2[at(other3 - lo2, eighth), :].astype(F32)).astype(BF16)
    ar3.start()
    dxacc[at(lo3, eighth), :] += rx2[at(lo3 - lo2, eighth), :].astype(F32)
    ar3.wait_recv()
    ybuf[at(lo3, eighth), :] = (dxacc[at(lo3, eighth), :] + rx3[...].astype(F32)).astype(BF16)
    backs = []
    for i, lo, size, partner in ((3, lo3, eighth, p3), (4, lo2, quarter, p2), (5, lo1, half, p1)):
        own_rows = ybuf.at[at(lo, size), :]
        back = ar_copy(i, own_rows, own_rows, partner)
        back.start()
        back.wait_recv()
        backs.append(back)
    dx_out[...] = ybuf[...]

    for c in range(max(0, chunks - 2), chunks):
        rs_mid(c)
    for c in range(chunks):
        rs_final(c)

    for copy in [ar1, ar2, ar3] + backs:
        copy.wait_send()
    for side, there in ((0, has_left), (1, has_right)):
        @pl.when(there)
        def _():
            for c in range(chunks):
                for kind in range(3):
                    ag_copy(own(c, kind), c, z, kind, side).wait_send()
    for d in range(1, n):
        for side in (0, 1):
            s = z - d if side == 0 else z + d
            here = (z >= d) if side == 0 else (z + d <= n - 1)
            onward = has_right if side == 0 else has_left
            @pl.when(jnp.logical_and(here, onward))
            def _():
                for c in range(chunks):
                    for kind in range(3):
                        ag_copy(slot(c, s, kind), c, s, kind, 1 - side).wait_send()
    for side in (0, 1):
        for k in rs_targets(side):
            sent = (k > z) if side else (k < z)
            @pl.when(sent)
            def _():
                for c in range(chunks):
                    rs_copy(c, k, side).wait_send()


def per_device_kernel(n, tokens, cotangent, gate_weight, up_weight, down_weight):
    rows, depth = tokens.shape
    shard, ff = gate_weight.shape
    chunks = ff // LANES
    vmem = pl.BlockSpec(memory_space=pltpu.VMEM)
    dma = pltpu.SemaphoreType.DMA
    return pl.pallas_call(
        functools.partial(kernel, n),
        out_shape=(jax.ShapeDtypeStruct((rows, depth), BF16),
                   jax.ShapeDtypeStruct((ff, shard), F32)),
        in_specs=[vmem] * 5,
        out_specs=(vmem, vmem),
        scratch_shapes=[
            pltpu.VMEM((depth, 2 * ff), BF16),
            pltpu.VMEM((n, ff, shard), BF16),
            pltpu.VMEM((n, rows, shard), BF16),
            pltpu.VMEM((rows, depth), F32),
            pltpu.VMEM((chunks, n, LANES, shard), F32),
            pltpu.VMEM((2, chunks, n, LANES, shard), BF16),
            pltpu.VMEM((2, chunks, n, LANES, shard), BF16),
            pltpu.VMEM((rows // 2, depth), BF16),
            pltpu.VMEM((rows // 4, depth), BF16),
            pltpu.VMEM((rows // 8, depth), BF16),
            pltpu.VMEM((rows // 2, depth), BF16),
            pltpu.VMEM((rows // 4, depth), BF16),
            pltpu.VMEM((rows // 8, depth), BF16),
            pltpu.VMEM((rows, depth), BF16),
            dma((2, chunks, n, 3)), dma((chunks, n, 3)),
            dma((2, chunks, n)), dma((2, chunks, n)),
            dma((6,)), dma((6,)), dma((chunks, 3)),
        ],
        compiler_params=pltpu.CompilerParams(
            collective_id=0, has_side_effects=True, vmem_limit_bytes=56 * 2**20),
    )(tokens, cotangent, gate_weight, up_weight, down_weight)


def solution(mesh):
    n, tp = mesh.shape["fs"], mesh.shape["tp"]

    def per_device(tokens, cotangent, gate_weight, up_weight, down_weight):
        rows = tokens.shape[0]
        shard, ff = gate_weight.shape
        args = (tokens, cotangent, gate_weight, up_weight, down_weight)
        fits = (tp == 8 and 2 <= n <= 8 and rows % (8 * SUB) == 0 and rows <= 512
                and shard % SUB == 0 and ff % LANES == 0)
        return per_device_kernel(n, *args) if fits else per_device_plain(*args)

    placed = (P("fs", None), P("fs", None), P("fs", "tp"), P("fs", "tp"), P("tp", "fs"))
    return jax.shard_map(
        per_device,
        mesh=mesh,
        in_specs=placed,
        out_specs=(P("fs", None), P("tp", "fs")),
        check_vma=False,
    )
```

```python
import functools

import jax
import jax.numpy as jnp
from jax import lax
from jax.experimental import pallas as pl
from jax.experimental.pallas import tpu as pltpu
from jax.sharding import PartitionSpec as P

LANES = 128
SUB = 16
BF16 = jnp.bfloat16
F32 = jnp.float32


def contract_rows(left, right):
    return lax.dot_general(
        left, right, (((0,), (0,)), ((), ())), preferred_element_type=jnp.float32
    )


def contract_cols(left, right):
    return lax.dot_general(
        left, right, (((1,), (1,)), ((), ())), preferred_element_type=jnp.float32
    )


def send_down(hidden, cotangent):
    return lax.psum_scatter(
        contract_rows(cotangent, hidden), "fs", scatter_dimension=0, tiled=True
    ).T


def per_device_plain(tokens, cotangent, gate_weight, up_weight, down_weight):
    whole_gate, whole_up, whole_down = (
        lax.all_gather(gate_weight, "fs", axis=0, tiled=True),
        lax.all_gather(up_weight, "fs", axis=0, tiled=True),
        lax.all_gather(down_weight, "fs", axis=1, tiled=True),
    )
    gate_pre = jnp.dot(tokens, whole_gate, preferred_element_type=jnp.float32)
    up_pre = jnp.dot(tokens, whole_up, preferred_element_type=jnp.float32)
    hidden_grad = contract_cols(cotangent, whole_down)
    sigmoid_gate = jax.nn.sigmoid(gate_pre)
    activated = gate_pre * sigmoid_gate
    hidden = (activated * up_pre).astype(jnp.bfloat16)
    gate_pre_grad = (
        hidden_grad * up_pre * sigmoid_gate * (1.0 + gate_pre * (1.0 - sigmoid_gate))
    ).astype(jnp.bfloat16)
    up_pre_grad = (hidden_grad * activated).astype(jnp.bfloat16)
    partial_value = contract_cols(gate_pre_grad, whole_gate) + contract_cols(up_pre_grad, whole_up)
    input_grad = lax.psum(partial_value.astype(jnp.bfloat16), "tp")
    down_grad = send_down(hidden, cotangent)
    return (input_grad, down_grad)


def kernel(n, tok_ref, cot_ref, gate_ref, up_ref, down_ref, dx_out, dg_out,
           wgu, wd, cot4, dxacc, part, rsr, rss, rx1, rx2, rx3, tx1, tx2, tx3, ybuf,
           ag_send, ag_recv, rs_send, rs_recv, ar_send, ar_recv, loc_sem):
    z = lax.axis_index("fs")
    b = lax.axis_index("tp")
    rows, depth = tok_ref.shape
    shard, ff = gate_ref.shape
    chunks = ff // LANES
    core = lax.rem(b, 2)
    m2 = 2 + 2 * core
    m3 = 6 - m2
    bit2 = lax.rem(b // m2, 2)
    bit3 = lax.rem(b // m3, 2)
    p1 = b + 1 - 2 * core
    p2 = b + m2 * (1 - 2 * bit2)
    p3 = b + m3 * (1 - 2 * bit3)
    has_left = z > 0
    has_right = z < n - 1

    def z_id(step):
        return {"fs": z + step}

    barrier = pltpu.get_barrier_semaphore()
    for partner in (p1, p2, p3):
        pl.semaphore_signal(barrier, inc=1, device_id={"tp": partner},
                            device_id_type=pl.DeviceIdType.MESH)
    for step, there in ((-1, has_left), (1, has_right)):
        @pl.when(there)
        def _():
            pl.semaphore_signal(barrier, inc=1, device_id=z_id(step),
                                device_id_type=pl.DeviceIdType.MESH)
    peers = 3 + lax.div(z + n - 1, n) + lax.div(2 * n - 2 - z, n)
    pl.semaphore_wait(barrier, peers)

    def slot(c, s, kind):
        r = pl.ds(pl.multiple_of(s * shard, SUB), shard)
        if kind == 0:
            return wgu.at[r, pl.ds(2 * c * LANES, LANES)]
        if kind == 1:
            return wgu.at[r, pl.ds((2 * c + 1) * LANES, LANES)]
        return wd.at[s, pl.ds(c * LANES, LANES), :]

    def own(c, kind):
        if kind == 0:
            return gate_ref.at[:, pl.ds(c * LANES, LANES)]
        if kind == 1:
            return up_ref.at[:, pl.ds(c * LANES, LANES)]
        return down_ref.at[pl.ds(c * LANES, LANES), :]

    def ag_copy(src, c, s, kind, side):
        step = 1 if side else -1
        return pltpu.make_async_remote_copy(
            src_ref=src, dst_ref=slot(c, s, kind),
            send_sem=ag_send.at[side, c, s, kind], recv_sem=ag_recv.at[c, s, kind],
            device_id=z_id(step), device_id_type=pl.DeviceIdType.MESH)

    def send_own(c):
        for side, there in ((0, has_left), (1, has_right)):
            @pl.when(there)
            def _():
                for kind in range(3):
                    ag_copy(own(c, kind), c, z, kind, side).start()

    def gather(c):
        for d in range(1, n):
            for side in (0, 1):
                s = z - d if side == 0 else z + d
                here = (z >= d) if side == 0 else (z + d <= n - 1)
                onward = has_right if side == 0 else has_left
                @pl.when(here)
                def _():
                    for kind in range(3):
                        src = slot(c, s, kind)
                        ag_copy(src, c, s, kind, 1 - side).wait_recv()
                        @pl.when(onward)
                        def _():
                            ag_copy(src, c, s, kind, 1 - side).start()

    def local_copy(c, kind):
        return pltpu.make_async_copy(own(c, kind), slot(c, z, kind), loc_sem.at[c, kind])

    for c in range(min(2, chunks)):
        send_own(c)
    for c in range(chunks):
        for kind in range(3):
            local_copy(c, kind).start()
    for k in range(n):
        cot4[k] = cot_ref[:, k * shard:(k + 1) * shard]

    def rs_copy(c, k, side):
        return pltpu.make_async_remote_copy(
            src_ref=rss.at[side, c, k], dst_ref=rsr.at[side, c, k],
            send_sem=rs_send.at[side, c, k], recv_sem=rs_recv.at[side, c, k],
            device_id=z_id(1 if side else -1), device_id_type=pl.DeviceIdType.MESH)

    def rs_targets(side):
        return range(n - 1, 0, -1) if side else range(n - 1)

    def rs_start(c):
        for side, end in ((1, z == 0), (0, z == n - 1)):
            @pl.when(end)
            def _():
                for k in rs_targets(side):
                    rss[side, c, k] = part[c, k].astype(BF16)
                    rs_copy(c, k, side).start()

    def rs_mid(c):
        for side, middle in ((1, has_left), (0, has_right)):
            for k in rs_targets(side):
                ahead = (k > z) if side else (k < z)
                @pl.when(jnp.logical_and(middle, ahead))
                def _():
                    rs_copy(c, k, side).wait_recv()
                    rss[side, c, k] = (part[c, k] + rsr[side, c, k].astype(F32)).astype(BF16)
                    rs_copy(c, k, side).start()

    def rs_final(c):
        r = pl.ds(c * LANES, LANES)
        dg_out[r, :] = part[c, z]
        for side, there in ((1, has_left), (0, has_right)):
            @pl.when(there)
            def _():
                rs_copy(c, z, side).wait_recv()
                dg_out[r, :] += rsr[side, c, z].astype(F32)

    def ar_copy(i, src, dst, partner):
        return pltpu.make_async_remote_copy(
            src_ref=src, dst_ref=dst, send_sem=ar_send.at[i], recv_sem=ar_recv.at[i],
            device_id={"tp": partner}, device_id_type=pl.DeviceIdType.MESH)

    half, quarter, eighth = rows // 2, rows // 4, rows // 8
    lo1 = core * half
    other1 = (1 - core) * half
    lo2 = lo1 + bit2 * quarter
    other2 = lo1 + (1 - bit2) * quarter
    lo3 = lo2 + bit3 * eighth
    other3 = lo2 + (1 - bit3) * eighth

    def at(lo, size):
        return pl.ds(pl.multiple_of(lo, SUB), size)

    ar1 = ar_copy(0, tx1, rx1, p1)
    ar2 = ar_copy(1, tx2, rx2, p2)
    ar3 = ar_copy(2, tx3, rx3, p3)

    for c in range(chunks):
        gather(c)
        if c + 2 < chunks:
            send_own(c + 2)
        if c >= 2:
            rs_mid(c - 2)
        for kind in range(3):
            local_copy(c, kind).wait()
        w = wgu[:, 2 * c * LANES:(2 * c + 2) * LANES]
        pre = jnp.dot(tok_ref[...], w, preferred_element_type=F32)
        hg = contract_cols(cot4[0], wd[0, c * LANES:(c + 1) * LANES, :])
        for k in range(1, n):
            hg += contract_cols(cot4[k], wd[k, c * LANES:(c + 1) * LANES, :])
        gate_pre, up_pre = pre[:, :LANES], pre[:, LANES:]
        sig = jax.nn.sigmoid(gate_pre)
        act = gate_pre * sig
        hidden = act * up_pre
        dgu = jnp.concatenate(
            [(hg * up_pre * sig * (1.0 + gate_pre * (1.0 - sig))).astype(BF16),
             (hg * act).astype(BF16)], axis=1)
        if c == 0:
            dxacc[...] = contract_cols(dgu, w)
        else:
            dxacc[...] += contract_cols(dgu, w)
        if c == chunks - 1:
            tx1[...] = dxacc[at(other1, half), :].astype(BF16)
            ar1.start()
        hidden_t = hidden.T.astype(BF16)
        for k in range(n):
            part[c, k] = jnp.dot(hidden_t, cot4[k], preferred_element_type=F32)
        rs_start(c)

    ar1.wait_recv()
    tx2[...] = (dxacc[at(other2, quarter), :]
                + rx1[at(other2 - lo1, quarter), :].astype(F32)).astype(BF16)
    ar2.start()
    dxacc[at(lo2, quarter), :] += rx1[at(lo2 - lo1, quarter), :].astype(F32)
    ar2.wait_recv()
    tx3[...] = (dxacc[at(other3, eighth), :]
                + rx2[at(other3 - lo2, eighth), :].astype(F32)).astype(BF16)
    ar3.start()
    dxacc[at(lo3, eighth), :] += rx2[at(lo3 - lo2, eighth), :].astype(F32)
    ar3.wait_recv()
    ybuf[at(lo3, eighth), :] = (dxacc[at(lo3, eighth), :] + rx3[...].astype(F32)).astype(BF16)
    backs = []
    for i, lo, size, partner in ((3, lo3, eighth, p3), (4, lo2, quarter, p2), (5, lo1, half, p1)):
        own_rows = ybuf.at[at(lo, size), :]
        back = ar_copy(i, own_rows, own_rows, partner)
        back.start()
        back.wait_recv()
        backs.append(back)
    dx_out[...] = ybuf[...]

    for c in range(max(0, chunks - 2), chunks):
        rs_mid(c)
    for c in range(chunks):
        rs_final(c)

    for copy in [ar1, ar2, ar3] + backs:
        copy.wait_send()
    for side, there in ((0, has_left), (1, has_right)):
        @pl.when(there)
        def _():
            for c in range(chunks):
                for kind in range(3):
                    ag_copy(own(c, kind), c, z, kind, side).wait_send()
    for d in range(1, n):
        for side in (0, 1):
            s = z - d if side == 0 else z + d
            here = (z >= d) if side == 0 else (z + d <= n - 1)
            onward = has_right if side == 0 else has_left
            @pl.when(jnp.logical_and(here, onward))
            def _():
                for c in range(chunks):
                    for kind in range(3):
                        ag_copy(slot(c, s, kind), c, s, kind, 1 - side).wait_send()
    for side in (0, 1):
        for k in rs_targets(side):
            sent = (k > z) if side else (k < z)
            @pl.when(sent)
            def _():
                for c in range(chunks):
                    rs_copy(c, k, side).wait_send()


def per_device_kernel(n, tokens, cotangent, gate_weight, up_weight, down_weight):
    rows, depth = tokens.shape
    shard, ff = gate_weight.shape
    chunks = ff // LANES
    vmem = pl.BlockSpec(memory_space=pltpu.VMEM)
    dma = pltpu.SemaphoreType.DMA
    return pl.pallas_call(
        functools.partial(kernel, n),
        out_shape=(jax.ShapeDtypeStruct((rows, depth), BF16),
                   jax.ShapeDtypeStruct((ff, shard), F32)),
        in_specs=[vmem] * 5,
        out_specs=(vmem, vmem),
        scratch_shapes=[
            pltpu.VMEM((depth, 2 * ff), BF16),
            pltpu.VMEM((n, ff, shard), BF16),
            pltpu.VMEM((n, rows, shard), BF16),
            pltpu.VMEM((rows, depth), F32),
            pltpu.VMEM((chunks, n, LANES, shard), F32),
            pltpu.VMEM((2, chunks, n, LANES, shard), BF16),
            pltpu.VMEM((2, chunks, n, LANES, shard), BF16),
            pltpu.VMEM((rows // 2, depth), BF16),
            pltpu.VMEM((rows // 4, depth), BF16),
            pltpu.VMEM((rows // 8, depth), BF16),
            pltpu.VMEM((rows // 2, depth), BF16),
            pltpu.VMEM((rows // 4, depth), BF16),
            pltpu.VMEM((rows // 8, depth), BF16),
            pltpu.VMEM((rows, depth), BF16),
            dma((2, chunks, n, 3)), dma((chunks, n, 3)),
            dma((2, chunks, n)), dma((2, chunks, n)),
            dma((6,)), dma((6,)), dma((chunks, 3)),
        ],
        compiler_params=pltpu.CompilerParams(
            collective_id=0, has_side_effects=True, vmem_limit_bytes=56 * 2**20),
    )(tokens, cotangent, gate_weight, up_weight, down_weight)


def solution(mesh):
    n, tp = mesh.shape["fs"], mesh.shape["tp"]

    def per_device(tokens, cotangent, gate_weight, up_weight, down_weight):
        rows = tokens.shape[0]
        shard, ff = gate_weight.shape
        args = (tokens, cotangent, gate_weight, up_weight, down_weight)
        fits = (tp == 8 and 2 <= n <= 8 and rows % (8 * SUB) == 0 and rows <= 512
                and shard % SUB == 0 and ff % LANES == 0)
        return per_device_kernel(n, *args) if fits else per_device_plain(*args)

    placed = (P("fs", None), P("fs", None), P("fs", "tp"), P("fs", "tp"), P("tp", "fs"))
    return jax.shard_map(
        per_device,
        mesh=mesh,
        in_specs=placed,
        out_specs=(P("fs", None), P("tp", "fs")),
        check_vma=False,
    )
```

```python
import functools

import jax
import jax.numpy as jnp
from jax import lax
from jax.experimental import pallas as pl
from jax.experimental.pallas import tpu as pltpu
from jax.sharding import PartitionSpec as P

LANES = 128
SUB = 16
BF16 = jnp.bfloat16
F32 = jnp.float32


def contract_rows(left, right):
    return lax.dot_general(
        left, right, (((0,), (0,)), ((), ())), preferred_element_type=jnp.float32
    )


def contract_cols(left, right):
    return lax.dot_general(
        left, right, (((1,), (1,)), ((), ())), preferred_element_type=jnp.float32
    )


def send_down(hidden, cotangent):
    return lax.psum_scatter(
        contract_rows(cotangent, hidden), "fs", scatter_dimension=0, tiled=True
    ).T


def per_device_plain(tokens, cotangent, gate_weight, up_weight, down_weight):
    whole_gate, whole_up, whole_down = (
        lax.all_gather(gate_weight, "fs", axis=0, tiled=True),
        lax.all_gather(up_weight, "fs", axis=0, tiled=True),
        lax.all_gather(down_weight, "fs", axis=1, tiled=True),
    )
    gate_pre = jnp.dot(tokens, whole_gate, preferred_element_type=jnp.float32)
    up_pre = jnp.dot(tokens, whole_up, preferred_element_type=jnp.float32)
    hidden_grad = contract_cols(cotangent, whole_down)
    sigmoid_gate = jax.nn.sigmoid(gate_pre)
    activated = gate_pre * sigmoid_gate
    hidden = (activated * up_pre).astype(jnp.bfloat16)
    gate_pre_grad = (
        hidden_grad * up_pre * sigmoid_gate * (1.0 + gate_pre * (1.0 - sigmoid_gate))
    ).astype(jnp.bfloat16)
    up_pre_grad = (hidden_grad * activated).astype(jnp.bfloat16)
    partial_value = contract_cols(gate_pre_grad, whole_gate) + contract_cols(up_pre_grad, whole_up)
    input_grad = lax.psum(partial_value.astype(jnp.bfloat16), "tp")
    down_grad = send_down(hidden, cotangent)
    return (input_grad, down_grad)


def kernel(n, tok_ref, cot_ref, gate_ref, up_ref, down_ref, dx_out, dg_out,
           weights, tok, cot, dxacc, part, rsr, rss, rx1, rx2, rx3, tx1, tx2, tx3, ybuf,
           ag_send, ag_recv, rs_send, rs_recv, ar_send, ar_recv, loc_sem):
    z = lax.axis_index("fs")
    b = lax.axis_index("tp")
    depth, rows = tok_ref.shape
    shard, ff = gate_ref.shape
    chunks = ff // LANES
    core = lax.rem(b, 2)
    m2 = 2 + 2 * core
    m3 = 6 - m2
    bit2 = lax.rem(b // m2, 2)
    bit3 = lax.rem(b // m3, 2)
    p1 = b + 1 - 2 * core
    p2 = b + m2 * (1 - 2 * bit2)
    p3 = b + m3 * (1 - 2 * bit3)
    has_left = z > 0
    has_right = z < n - 1

    def z_id(step):
        return {"fs": z + step}

    barrier = pltpu.get_barrier_semaphore()
    for partner in (p1, p2, p3):
        pl.semaphore_signal(barrier, inc=1, device_id={"tp": partner},
                            device_id_type=pl.DeviceIdType.MESH)
    for step, there in ((-1, has_left), (1, has_right)):
        @pl.when(there)
        def _():
            pl.semaphore_signal(barrier, inc=1, device_id=z_id(step),
                                device_id_type=pl.DeviceIdType.MESH)
    peers = 3 + lax.div(z + n - 1, n) + lax.div(2 * n - 2 - z, n)
    pl.semaphore_wait(barrier, peers)

    def slot(c, s, kind):
        r = pl.ds(pl.multiple_of(s * shard, SUB), shard)
        return weights.at[r, pl.ds((3 * c + kind) * LANES, LANES)]

    def own(c, kind):
        return (gate_ref, up_ref, down_ref)[kind].at[:, pl.ds(c * LANES, LANES)]

    def ag_copy(src, c, s, kind, side):
        step = 1 if side else -1
        return pltpu.make_async_remote_copy(
            src_ref=src, dst_ref=slot(c, s, kind),
            send_sem=ag_send.at[side, c, s, kind], recv_sem=ag_recv.at[c, s, kind],
            device_id=z_id(step), device_id_type=pl.DeviceIdType.MESH)

    def send_own(c):
        for side, there in ((0, has_left), (1, has_right)):
            @pl.when(there)
            def _():
                for kind in range(3):
                    ag_copy(own(c, kind), c, z, kind, side).start()

    def gather(c):
        for d in range(1, n):
            for side in (0, 1):
                s = z - d if side == 0 else z + d
                here = (z >= d) if side == 0 else (z + d <= n - 1)
                onward = has_right if side == 0 else has_left
                @pl.when(here)
                def _():
                    for kind in range(3):
                        src = slot(c, s, kind)
                        ag_copy(src, c, s, kind, 1 - side).wait_recv()
                        @pl.when(onward)
                        def _():
                            ag_copy(src, c, s, kind, 1 - side).start()

    def local_copy(c, kind):
        return pltpu.make_async_copy(own(c, kind), slot(c, z, kind), loc_sem.at[c, kind])

    for c in range(min(2, chunks)):
        send_own(c)
    for c in range(chunks):
        for kind in range(3):
            local_copy(c, kind).start()
    tok[...] = tok_ref[...].T
    cot[...] = cot_ref[...].T

    def rs_copy(c, k, side):
        return pltpu.make_async_remote_copy(
            src_ref=rss.at[side, c, k], dst_ref=rsr.at[side, c, k],
            send_sem=rs_send.at[side, c, k], recv_sem=rs_recv.at[side, c, k],
            device_id=z_id(1 if side else -1), device_id_type=pl.DeviceIdType.MESH)

    def rs_targets(side):
        return range(n - 1, 0, -1) if side else range(n - 1)

    def rs_start(c):
        for side, end in ((1, z == 0), (0, z == n - 1)):
            @pl.when(end)
            def _():
                for k in rs_targets(side):
                    rss[side, c, k] = part[c, k].astype(BF16)
                    rs_copy(c, k, side).start()

    def rs_mid(c):
        for side, middle in ((1, has_left), (0, has_right)):
            for k in rs_targets(side):
                ahead = (k > z) if side else (k < z)
                @pl.when(jnp.logical_and(middle, ahead))
                def _():
                    rs_copy(c, k, side).wait_recv()
                    rss[side, c, k] = (part[c, k] + rsr[side, c, k].astype(F32)).astype(BF16)
                    rs_copy(c, k, side).start()

    def rs_final(c):
        r = pl.ds(c * LANES, LANES)
        dg_out[:, r] = part[c, z]
        for side, there in ((1, has_left), (0, has_right)):
            @pl.when(there)
            def _():
                rs_copy(c, z, side).wait_recv()
                dg_out[:, r] += rsr[side, c, z].astype(F32)

    def ar_copy(i, src, dst, partner):
        return pltpu.make_async_remote_copy(
            src_ref=src, dst_ref=dst, send_sem=ar_send.at[i], recv_sem=ar_recv.at[i],
            device_id={"tp": partner}, device_id_type=pl.DeviceIdType.MESH)

    half, quarter, lanes = depth // 2, depth // 4, rows // 2
    lo1 = core * half
    other1 = (1 - core) * half
    lo2 = lo1 + bit2 * quarter
    other2 = lo1 + (1 - bit2) * quarter
    mine3 = pl.ds(pl.multiple_of(bit3 * lanes, LANES), lanes)
    other3 = pl.ds(pl.multiple_of((1 - bit3) * lanes, LANES), lanes)

    def at(lo, size):
        return pl.ds(pl.multiple_of(lo, SUB), size)

    ar1 = ar_copy(0, tx1, rx1, p1)
    ar2 = ar_copy(1, tx2, rx2, p2)
    ar3 = ar_copy(2, tx3, rx3, p3)

    for c in range(chunks):
        gather(c)
        if c + 2 < chunks:
            send_own(c + 2)
        if c >= 2:
            rs_mid(c - 2)
        for kind in range(3):
            local_copy(c, kind).wait()
        w = weights[:, 3 * c * LANES:(3 * c + 2) * LANES]
        pre = jnp.dot(tok[...], w, preferred_element_type=F32)
        hg = jnp.dot(cot[...], weights[:, (3 * c + 2) * LANES:(3 * c + 3) * LANES],
                     preferred_element_type=F32)
        gate_pre, up_pre = pre[:, :LANES], pre[:, LANES:]
        sig = jax.nn.sigmoid(gate_pre)
        act = gate_pre * sig
        hidden = (act * up_pre).astype(BF16)
        dgu = jnp.concatenate(
            [(hg * up_pre * sig * (1.0 + gate_pre * (1.0 - sig))).astype(BF16),
             (hg * act).astype(BF16)], axis=1)
        if c == 0:
            dxacc[...] = contract_cols(w, dgu)
        else:
            dxacc[...] += contract_cols(w, dgu)
        if c == chunks - 1:
            tx1[...] = dxacc[at(other1, half), :].astype(BF16)
            ar1.start()
        for k in range(n):
            part[c, k] = jnp.dot(cot_ref[k * shard:(k + 1) * shard, :], hidden,
                                 preferred_element_type=F32)
        rs_start(c)

    ar1.wait_recv()
    tx2[...] = (dxacc[at(other2, quarter), :]
                + rx1[at(other2 - lo1, quarter), :].astype(F32)).astype(BF16)
    ar2.start()
    dxacc[at(lo2, quarter), :] += rx1[at(lo2 - lo1, quarter), :].astype(F32)
    ar2.wait_recv()
    q = at(lo2, quarter)
    tx3[...] = (dxacc[q, other3] + rx2[:, other3].astype(F32)).astype(BF16)
    ar3.start()
    kept = dxacc[q, mine3] + rx2[:, mine3].astype(F32)
    ar3.wait_recv()
    ybuf[q, mine3] = (kept + rx3[...].astype(F32)).astype(BF16)
    backs = []
    whole = pl.ds(0, rows)
    for i, r, l, partner in ((3, q, mine3, p3), (4, q, whole, p2), (5, at(lo1, half), whole, p1)):
        own_rows = ybuf.at[r, l]
        back = ar_copy(i, own_rows, own_rows, partner)
        back.start()
        back.wait_recv()
        backs.append(back)
    dx_out[...] = ybuf[...]

    for c in range(max(0, chunks - 2), chunks):
        rs_mid(c)
    for c in range(chunks):
        rs_final(c)

    for copy in [ar1, ar2, ar3] + backs:
        copy.wait_send()
    for side, there in ((0, has_left), (1, has_right)):
        @pl.when(there)
        def _():
            for c in range(chunks):
                for kind in range(3):
                    ag_copy(own(c, kind), c, z, kind, side).wait_send()
    for d in range(1, n):
        for side in (0, 1):
            s = z - d if side == 0 else z + d
            here = (z >= d) if side == 0 else (z + d <= n - 1)
            onward = has_right if side == 0 else has_left
            @pl.when(jnp.logical_and(here, onward))
            def _():
                for c in range(chunks):
                    for kind in range(3):
                        ag_copy(slot(c, s, kind), c, s, kind, 1 - side).wait_send()
    for side in (0, 1):
        for k in rs_targets(side):
            sent = (k > z) if side else (k < z)
            @pl.when(sent)
            def _():
                for c in range(chunks):
                    rs_copy(c, k, side).wait_send()


def per_device_kernel(n, tokens, cotangent, gate_weight, up_weight, down_weight):
    rows, depth = tokens.shape
    shard, ff = gate_weight.shape
    chunks = ff // LANES
    vmem = pl.BlockSpec(memory_space=pltpu.VMEM)
    dma = pltpu.SemaphoreType.DMA
    dx, dg = pl.pallas_call(
        functools.partial(kernel, n),
        out_shape=(jax.ShapeDtypeStruct((depth, rows), BF16),
                   jax.ShapeDtypeStruct((shard, ff), F32)),
        in_specs=[vmem] * 5,
        out_specs=(vmem, vmem),
        scratch_shapes=[
            pltpu.VMEM((depth, 3 * ff), BF16),
            pltpu.VMEM((rows, depth), BF16),
            pltpu.VMEM((rows, depth), BF16),
            pltpu.VMEM((depth, rows), F32),
            pltpu.VMEM((chunks, n, shard, LANES), F32),
            pltpu.VMEM((2, chunks, n, shard, LANES), BF16),
            pltpu.VMEM((2, chunks, n, shard, LANES), BF16),
            pltpu.VMEM((depth // 2, rows), BF16),
            pltpu.VMEM((depth // 4, rows), BF16),
            pltpu.VMEM((depth // 4, rows // 2), BF16),
            pltpu.VMEM((depth // 2, rows), BF16),
            pltpu.VMEM((depth // 4, rows), BF16),
            pltpu.VMEM((depth // 4, rows // 2), BF16),
            pltpu.VMEM((depth, rows), BF16),
            dma((2, chunks, n, 3)), dma((chunks, n, 3)),
            dma((2, chunks, n)), dma((2, chunks, n)),
            dma((6,)), dma((6,)), dma((chunks, 3)),
        ],
        compiler_params=pltpu.CompilerParams(
            collective_id=0, has_side_effects=True, vmem_limit_bytes=56 * 2**20),
    )(tokens.T, cotangent.T, gate_weight, up_weight, down_weight.T)
    return dx.T, dg.T


def solution(mesh):
    n, tp = mesh.shape["fs"], mesh.shape["tp"]

    def per_device(tokens, cotangent, gate_weight, up_weight, down_weight):
        rows = tokens.shape[0]
        shard, ff = gate_weight.shape
        args = (tokens, cotangent, gate_weight, up_weight, down_weight)
        fits = (tp == 8 and 2 <= n <= 8 and rows % (2 * LANES) == 0 and tokens.shape[1] % (4 * SUB) == 0 and rows <= 512
                and shard % SUB == 0 and ff % LANES == 0)
        return per_device_kernel(n, *args) if fits else per_device_plain(*args)

    placed = (P("fs", None), P("fs", None), P("fs", "tp"), P("fs", "tp"), P("tp", "fs"))
    return jax.shard_map(
        per_device,
        mesh=mesh,
        in_specs=placed,
        out_specs=(P("fs", None), P("tp", "fs")),
        check_vma=False,
    )
```
